128 devices in a mesh: ep: 16 (over z, x), tp: 8 (over y, core).
Axes of the slice: x: 4, y: 4, z: 4, core: 2. Of those that a mesh axis runs over, the one named last changes fastest.
Arguments:
- tokens: bfloat16 [16384, 2048], P(('ep', 'tp')), may hold values from -6 to 6
- expert_ids: int32 [16384, 4], P('ep'), may hold values from 0 to 15, all different within a row; in each aligned block of 128 rows (0 to 127, 128 to 255, ...) at most 64 rows name the same one
- gate_values: float32 [16384, 4], P('ep'), may hold values from 0.1 to 1
- norm_gain: float32 [2048], replicated, may hold values from 0.1 to 1.9
- gate_weight: bfloat16 [16, 2048, 1024], P('ep', None, 'tp'), may hold values from -0.125 to 0.125
- up_weight: bfloat16 [16, 2048, 1024], P('ep', None, 'tp'), may hold values from -0.125 to 0.125
- down_weight: bfloat16 [16, 1024, 2048], P('ep', 'tp'), may hold values from -0.1875 to 0.1875
- out_gain: float32 [2048], P('tp'), may hold values from 0.1 to 1.9
Outputs:
- mixed: bfloat16 [16384, 2048], P('ep', 'tp')
The draws below stay inside these ranges and needn't reach their ends.
Inputs may be any that keep to these rules, and one draw needn't show every extreme that they name: `expert_ids`: each row names 4 different experts of 0 to 15; within the rows of one device (aligned blocks of 128 rows) no expert is named more than 64 times, and in some blocks one expert is named exactly 64 times.
All inputs are finite; a program needn't handle non-finite values.
Results may differ from the reference program's by a relative error of at most 0.0025.
Values may be sent and summed in bfloat16 or wider, within the bound.
A program may use at most 64 MiB of HBM per device.

```python
import math
import jax
import jax.numpy as jnp
import numpy as np
from jax import lax

D = 2048
FF = 1024
TOP = 4
TOK_DEV = 128
CAP = 64
EXPERTS = 16
TOKENS = 16384
N_EP = 16
N_TP = 8


def level_of(rng, extent, split, least, largest):
    factor_of = 1.0
    for dim, parts in split:
        heights = jax.random.uniform(jax.random.fold_in(jax.random.fold_in(rng, 6), dim), (parts,), jnp.float32, least / len(split), largest / len(split))
        factor_of = factor_of * jnp.repeat(jnp.exp(heights), extent[dim] // parts).reshape((-1,) + (1,) * (len(extent) - 1 - dim))
    return factor_of


def routed_block(own_key, own, number, rows, count, top, limit, lean):
    order = jax.random.permutation(own_key, count)
    heavy_load, usual = load_shares(count, rows * top, limit, lean, True), load_shares(count, rows * top, limit, lean, False)
    places = jnp.arange(count)

    def named(tallies, rotation):
        used = int((tallies > 0).sum())
        fixed = max(1, used // 4)
        shifted = fixed + (places - fixed + rotation * (used - fixed)) % max(1, count - fixed)
        return jnp.zeros((count,), jnp.int32).at[order[jnp.where(places < fixed, places, shifted)]].set(jnp.asarray(tallies, jnp.int32))

    tallies = jnp.where(number % 4 == 0, named(heavy_load, number // 4), named(usual, number - number // 4 - 1))
    mixed = jax.random.permutation(jax.random.fold_in(own, 3), count)
    source_of, sink = mixed[0:count // 2 * 2:2], mixed[1:count // 2 * 2:2]
    slack = jnp.minimum(tallies[source_of] - 1, limit - tallies[sink]) // 2
    slack = jnp.where((source_of == order[0]) | (sink == order[0]) | (tallies[sink] == 0), 0, jnp.maximum(slack, 0))
    shifted = jax.random.randint(jax.random.fold_in(own, 4), (count // 2,), 0, 1 << 20) % (slack + 1)
    tallies = tallies.at[source_of].add(-shifted).at[sink].add(shifted)
    items = jnp.searchsorted(jnp.cumsum(tallies), jnp.arange(rows * top), side="right").astype(jnp.int32)
    table = items.reshape(top, rows).T
    table = table[jax.random.permutation(jax.random.fold_in(own, 1), rows)]
    rotation = jax.random.randint(jax.random.fold_in(own, 2), (rows, 1), 0, top)
    return jnp.take_along_axis(table, (jnp.arange(top)[None, :] + rotation) % top, axis=1)


def load_shares(number_of, total, limit, lean, full):
    portions = [(1 << 20) // math.isqrt(standing ** lean) + 1 for standing in range(1, number_of + 1)]
    largest = limit if full else min(limit, max(-(-total // number_of), total * portions[0] // sum(portions)))
    least = 1 if total - largest >= number_of - 1 else 0
    given, surplus = [largest] + [least] * (number_of - 1), total - largest - least * (number_of - 1)
    while surplus > 0:
        candidates = [i for i in range(1, number_of) if given[i] < largest] or [i for i in range(1, number_of) if given[i] < limit]
        mass, left = sum([portions[i] for i in candidates]), surplus
        for i in candidates:
            addition = min(limit - given[i], max(1, left * portions[i] // mass), surplus)
            given[i] = given[i] + addition
            surplus = surplus - addition
    return np.array(given)


def centred(key, dims, width, bound, pieces=(), held_as=jnp.bfloat16):
    values = width * jax.random.normal(key, dims, jnp.float32)
    if pieces:
        values = values * level_of(key, dims, pieces, -0.22, 0.18)
    return jnp.clip(values, -bound, bound).astype(held_as)


def setup_inputs(seed: int = 0) -> dict:
    key_of = jax.random.split(jax.random.key(seed), 9)
    tokens = centred(key_of[0], (TOKENS, D), 1.0, 6.0, ((0, 128),))
    expert_ids_keys = jax.random.split(jax.random.fold_in(key_of[1], 1), TOKENS // TOK_DEV)
    expert_ids_turns = jax.random.permutation(jax.random.fold_in(key_of[1], 3), TOKENS // TOK_DEV)
    expert_ids = jax.vmap(lambda own, number: routed_block(jax.random.fold_in(key_of[1], 2), own, number, TOK_DEV, EXPERTS, TOP, CAP, 2))(expert_ids_keys, expert_ids_turns).reshape((TOKENS, TOP))
    gate_values = jnp.clip(0.1 + 0.9 * jax.random.uniform(key_of[2], (TOKENS, TOP), jnp.float32) ** level_of(key_of[2], (TOKENS, TOP), ((0, 16),), -0.2, 0.2), 0.1, 1.0)
    norm_gain = jnp.clip(1.0 + 0.18 * jax.random.normal(key_of[3], (D,), jnp.float32), 0.1, 1.9)
    gate_weight = centred(key_of[4], (EXPERTS, D, FF), D ** -0.5, 0.125, ((0, 16), (2, 8)))
    up_weight = centred(key_of[5], (EXPERTS, D, FF), D ** -0.5, 0.125, ((0, 16), (2, 8)))
    down_weight = centred(key_of[6], (EXPERTS, FF, D), FF ** -0.5, 0.1875, ((0, 16), (1, 8)))
    out_gain = jnp.clip(1.0 + 0.18 * jax.random.normal(key_of[7], (D,), jnp.float32), 0.1, 1.9)
    return dict(tokens=tokens, expert_ids=expert_ids, gate_values=gate_values, norm_gain=norm_gain, gate_weight=gate_weight, up_weight=up_weight, down_weight=down_weight, out_gain=out_gain)


epsilon = 1e-05
clamp_limit = 7.0
sigmoid_alpha = 1.702

def rms_rows(values, gain):
    mean_sq = lax.optimization_barrier(jnp.mean(values * values, axis=-1, keepdims=True))
    return values * lax.rsqrt(mean_sq + epsilon) * gain

def clamped_unit(gate_part, up_part):
    glu_part = jnp.minimum(gate_part, clamp_limit)
    lin_part = jnp.clip(up_part, -clamp_limit, clamp_limit)
    return glu_part * jax.nn.sigmoid(sigmoid_alpha * glu_part) * (lin_part + 1.0)

def reference(tokens, expert_ids, gate_values, norm_gain, gate_weight, up_weight, down_weight, out_gain):
    normed = rms_rows(tokens.astype(jnp.float32), norm_gain).astype(jnp.bfloat16)
    blocks = expert_ids.reshape(N_EP * N_TP, TOK_DEV * TOP)
    onehot = (blocks[:, :, None] == jnp.arange(EXPERTS, dtype=jnp.int32)[None, None, :]).astype(jnp.int32)
    slot_num = lax.optimization_barrier(jnp.sum((jnp.cumsum(onehot, axis=1) - onehot) * onehot, axis=2)).reshape(TOKENS, TOP)
    source = (jnp.arange(TOKENS, dtype=jnp.int32) // TOK_DEV)[:, None]
    position = (source * CAP + slot_num).astype(jnp.int32)
    table_rows = N_EP * N_TP * CAP
    token_index = jnp.broadcast_to(jnp.arange(TOKENS, dtype=jnp.int32)[:, None], (TOKENS, TOP)).reshape(-1)
    padded = jnp.concatenate([normed, jnp.zeros((1, D), jnp.bfloat16)], axis=0)

    def one_expert(running, inputs):
        expert, w_gate, w_up, w_down = inputs
        chosen = expert_ids == expert
        where_row = jnp.where(chosen, position, table_rows).astype(jnp.int32)
        owner_row = jnp.full((table_rows + 1,), TOKENS, jnp.int32).at[where_row.reshape(-1)].set(token_index)
        rows_in = padded[owner_row[:table_rows]].astype(jnp.float32)
        gate_part = jnp.dot(rows_in, w_gate.astype(jnp.float32), precision=lax.Precision.HIGHEST)
        up_part = jnp.dot(rows_in, w_up.astype(jnp.float32), precision=lax.Precision.HIGHEST)
        activated = clamped_unit(gate_part, up_part).astype(jnp.bfloat16)
        activated = lax.optimization_barrier(activated).astype(jnp.float32)
        outputs = jnp.dot(activated, w_down.astype(jnp.float32), precision=lax.Precision.HIGHEST).astype(jnp.bfloat16)
        outputs = lax.optimization_barrier(outputs).astype(jnp.float32)
        outputs = jnp.concatenate([outputs, jnp.zeros((1, D), jnp.float32)], axis=0)
        for choice_k in range(TOP):
            weight = jnp.where(chosen[:, choice_k], gate_values[:, choice_k], jnp.float32(0.0))
            running = running + weight[:, None] * outputs[where_row[:, choice_k]]
        return (running, None)
    combined, _ = lax.scan(one_expert, jnp.zeros((TOKENS, D), jnp.float32), (jnp.arange(EXPERTS, dtype=jnp.int32), gate_weight, up_weight, down_weight))
    mean_sq = lax.optimization_barrier(jnp.mean(combined * combined, axis=1, keepdims=True))
    return (combined * lax.rsqrt(mean_sq + epsilon) * out_gain).astype(jnp.bfloat16)
```

```python
import jax
import jax.numpy as jnp
from jax import lax
from jax.experimental import pallas as pl
from jax.experimental.pallas import tpu as pltpu
from jax.sharding import PartitionSpec as P

epsilon = 1e-05
clamp_limit = 7.0
sigmoid_alpha = 1.702

MESH = pl.DeviceIdType.MESH
F32, BF16 = jnp.float32, jnp.bfloat16
D, FF, TOP, TOK, CAP = 2048, 1024, 4, 128, 64
NE, NT = 16, 8
HID = FF // NT
NCH = 4
CW = D // NCH
SL = D // NT
DA = (0, 1, 3, 2)


def clamped_unit(gate_part, up_part):
    glu_part = jnp.minimum(gate_part, clamp_limit)
    lin_part = jnp.clip(up_part, -clamp_limit, clamp_limit)
    return glu_part * jax.nn.sigmoid(sigmoid_alpha * glu_part) * (lin_part + 1.0)


def kernel(
    tok_ref, ids_ref, gv_ref, gain_ref, g_ref, u_ref, d_ref, og_ref,
    out_ref,
    wgu, wd, tb, rt, sel, xr, act, ob, rb, ret, comb, cm, mixed, og,
    w_own, w_s, w_r, d_s, d_r, s1_s, s1_r, s2_s, s2_r, r1_s, r1_r, r2_s, r2_r, g_s, g_r, o_s, o_r, o_l,
):
    ep, tp = lax.axis_index("ep"), lax.axis_index("tp")
    z, x = ep // 4, ep % 4
    y, c = tp // 2, tp % 2
    a = z * (1 - c) + x * c
    b = x * (1 - c) + z * c
    wa, wb = 4 - 3 * c, 1 + 3 * c

    def ab(da, db):
        return (((a + da) % 4) * wa + ((b + db) % 4) * wb, tp)

    def yc(dy, dc):
        return (ep, ((y + dy) % 4) * 2 + (c + dc) % 2)

    def send(src, dst, ss, rs, dev):
        cp = pltpu.make_async_remote_copy(
            src_ref=src, dst_ref=dst, send_sem=ss, recv_sem=rs, device_id=dev, device_id_type=MESH
        )
        return cp

    sent = []

    def go(cp):
        cp.start()
        sent.append(cp)
        return cp

    barrier = pltpu.get_barrier_semaphore()
    peers = [ab(i, 0) for i in (1, 2, 3)] + [ab(0, i) for i in (1, 2, 3)]
    peers += [(ep, (tp + i) % NT) for i in range(1, NT)]
    for peer in peers:
        pl.semaphore_signal(barrier, inc=1, device_id=peer, device_id_type=MESH)
    pl.semaphore_wait(barrier, len(peers))

    def gview(p, i):
        return wgu.at[p, :, pl.ds(i * 256, 128)]

    def uview(p, i):
        return wgu.at[p, :, pl.ds(i * 256 + 128, 128)]

    def dview(j, p, i, lo=0, n=HID):
        return wd.at[j, pl.ds((2 * p + i) * HID + lo, n), :]

    gin, uin = g_ref.at[0], u_ref.at[0]

    def din(j):
        return d_ref.at[0, :, pl.ds(j * CW, CW)]

    def wsem(kind, p, i):
        return kind * 8 + i * 4 + p

    def wcopy(kind, src, p, i, dev, extra=0):
        view = gview if kind == 0 else uview
        k = wsem(kind, p, i)
        return send(src, view(p, i), w_s.at[k], w_r.at[k], dev)

    up1, up2 = yc(1, 0), yc(3, 0)
    sib = yc(0, 1)
    g_up = go(wcopy(0, gin, 2, 0, up1))
    g_dn = go(wcopy(0, gin, 1, 0, up2))
    u_up = go(wcopy(1, uin, 2, 0, up1))
    u_dn = go(wcopy(1, uin, 1, 0, up2))
    g_sib = go(wcopy(0, gin, 0, 1, sib))
    u_sib = go(wcopy(1, uin, 0, 1, sib))
    locs = [
        pltpu.make_async_copy(gin, gview(0, 0), w_own.at[0]),
        pltpu.make_async_copy(uin, uview(0, 0), w_own.at[1]),
    ]
    for j in range(NCH):
        locs.append(pltpu.make_async_copy(din(j), dview(j, 0, 0), w_own.at[2 + j]))
    for cp in locs:
        cp.start()
    ogc = []
    for i in range(1, NT):
        ogc.append(go(send(og_ref, og.at[tp], g_s.at[i - 1], g_r.at[i - 1], (ep, (tp + i) % NT))))
    og[tp] = og_ref[...]

    tf = tok_ref[...].astype(F32)
    ms = jnp.mean(tf * tf, axis=-1, keepdims=True)
    tb[0] = (tf * lax.rsqrt(ms + epsilon) * gain_ref[...]).astype(BF16)

    q = lax.broadcasted_iota(jnp.int32, (NE, TOK), 0)
    eid = ((a + q // 4) % 4) * wa + ((b + q % 4) % 4) * wb
    off = pl.multiple_of(tp * TOK, TOK)
    named = jnp.zeros((NE, TOK), F32)
    weight = jnp.zeros((NE, TOK), F32)
    for k in range(TOP):
        hit = ids_ref[k : k + 1, pl.ds(off, TOK)] == eid
        named = named + jnp.where(hit, 1.0, 0.0)
        weight = weight + jnp.where(hit, gv_ref[k : k + 1, pl.ds(off, TOK)], 0.0)
    tri = lax.broadcasted_iota(jnp.int32, (TOK, TOK), 0) < lax.broadcasted_iota(jnp.int32, (TOK, TOK), 1)
    earlier = jnp.dot(named.astype(BF16), jnp.where(tri, 1.0, 0.0).astype(BF16), preferred_element_type=F32)
    table = jnp.where(named > 0.5, earlier, -1.0)
    rt[0] = table

    s1 = {}
    for n, da in enumerate((1, 3, 2)):
        s1[da] = (
            send(tb.at[0], tb.at[(4 - da) % 4], s1_s.at[2 * n], s1_r.at[2 * ((4 - da) % 4)], ab(da, 0)),
            send(rt.at[0], rt.at[(4 - da) % 4], s1_s.at[2 * n + 1], s1_r.at[2 * ((4 - da) % 4) + 1], ab(da, 0)),
        )
        go(s1[da][1])
        go(s1[da][0])

    slot_iota = lax.broadcasted_iota(jnp.int32, (CAP, TOK), 0).astype(F32)

    s2 = {}

    def select(g):
        da = DA[g]
        rows = tb[da]
        for db in range(4):
            line = rt[da, ((4 - da) % 4) * 4 + db : ((4 - da) % 4) * 4 + db + 1, :]
            pick = jnp.where(line == slot_iota, 1.0, 0.0).astype(BF16)
            got = jnp.dot(pick, rows, preferred_element_type=F32).astype(BF16)
            if db == 0:
                xr[g, 0] = got
            else:
                sel[g, db - 1] = got
        for db in (1, 3, 2):
            k, kr = g * 3 + db - 1, g * 3 + (4 - db) % 4 - 1
            s2[g, db] = go(
                send(sel.at[g, db - 1], xr.at[g, (4 - db) % 4], s2_s.at[k], s2_r.at[kr], ab(0, db))
            )

    select(0)

    pad = jnp.zeros((TOK - NE, TOK), F32)
    table_t = jnp.concatenate([table, pad], axis=0).T[:, :NE]
    weight_t = jnp.concatenate([weight, pad], axis=0).T[:, :NE]
    spread = (
        lax.broadcasted_iota(jnp.int32, (NE, NE * CAP), 1) // CAP
        == lax.broadcasted_iota(jnp.int32, (NE, NE * CAP), 0)
    )
    spread = jnp.where(spread, 1.0, 0.0).astype(BF16)
    slot_of = jnp.dot(table_t.astype(BF16), spread, preferred_element_type=F32)
    lane_slot = (lax.broadcasted_iota(jnp.int32, (TOK, NE * CAP), 1) % CAP).astype(F32)
    here = slot_of == lane_slot
    rest = weight_t
    for i in range(3):
        part = rest.astype(BF16)
        rest = rest - part.astype(F32)
        wide = jnp.dot(part, spread, preferred_element_type=F32)
        cm[i * TOK : (i + 1) * TOK, :] = jnp.where(here, wide, 0.0).astype(BF16)

    def s1_wait(da):
        n = {1: 0, 3: 1, 2: 2}[da]
        for t, buf in ((1, rt), (0, tb)):
            send(buf.at[0], buf.at[da], s1_s.at[2 * n + t], s1_r.at[2 * da + t], ab(da, 0)).wait_recv()

    s1_wait(1)
    select(1)
    s1_wait(3)
    select(2)

    def w_wait(kind, p, i):
        wcopy(kind, gin if kind == 0 else uin, p, i, sib).wait_recv()

    def to_sib(kind, p):
        view = gview if kind == 0 else uview
        go(wcopy(kind, view(p, 0), p, 1, sib))

    def gu(g, p):
        rows = xr[g].reshape(4 * CAP, D)
        h = jnp.dot(rows, wgu[p], preferred_element_type=F32)
        for i in range(2):
            part = clamped_unit(h[:, i * 256 : i * 256 + 128], h[:, i * 256 + 128 : i * 256 + 256])
            act[g, :, pl.ds(pl.multiple_of((2 * p + i) * HID, HID), HID)] = part.astype(BF16)

    def x_wait(g):
        for db in (1, 3, 2):
            s2w = send(sel.at[g, db - 1], xr.at[g, db], s2_s.at[g * 3 + db - 1], s2_r.at[g * 3 + db - 1], ab(0, db))
            s2w.wait_recv()

    w_wait(0, 2, 0)
    go(wcopy(0, gview(2, 0), 3, 0, up1))
    to_sib(0, 2)
    w_wait(0, 1, 0)
    to_sib(0, 1)
    s1_wait(2)
    select(3)

    locs[0].wait()
    locs[1].wait()
    w_wait(0, 0, 1)
    w_wait(1, 0, 1)
    x_wait(0)
    gu(0, 0)

    def dsem(j, p, i):
        return j * 9 + p * 2 + i

    def dcopy(j, src, p, i, dev, lo=0, n=HID):
        k = dsem(j, p, i) if lo == 0 else j * 9 + 8
        return send(src, dview(j, p, i, lo, n), d_s.at[k], d_r.at[k], dev)

    def d_start(j):
        go(dcopy(j, din(j), 2, 0, up1))
        go(dcopy(j, din(j), 1, 0, up2))
        go(dcopy(j, din(j), 0, 1, sib))

    def d_fwd(j):
        dcopy(j, din(j), 2, 0, sib).wait_recv()
        go(dcopy(j, dview(j, 2, 0, 0, 64), 3, 0, up1, 0, 64))
        dcopy(j, din(j), 1, 0, sib).wait_recv()
        go(dcopy(j, dview(j, 1, 0, 64, 64), 3, 0, up2, 64, 64))
        go(dcopy(j, dview(j, 2, 0), 2, 1, sib))
        go(dcopy(j, dview(j, 1, 0), 1, 1, sib))

    def d_last(j):
        dcopy(j, dview(j, 2, 0, 0, 64), 3, 0, sib, 0, 64).wait_recv()
        dcopy(j, dview(j, 1, 0, 64, 64), 3, 0, sib, 64, 64).wait_recv()
        go(dcopy(j, dview(j, 3, 0), 3, 1, sib))

    def d_all(j):
        locs[2 + j].wait()
        for p in range(4):
            dcopy(j, din(j), p, 1, sib).wait_recv()

    w_wait(1, 1, 0)
    go(wcopy(1, uview(1, 0), 3, 0, up2))
    to_sib(1, 1)
    w_wait(1, 2, 0)
    to_sib(1, 2)
    d_start(0)
    d_start(1)
    x_wait(1)
    for p in (1, 2):
        w_wait(0, p, 1)
        w_wait(1, p, 1)

    @pl.loop(1, 3)
    def _(p):
        gu(0, p)

    @pl.loop(0, 3)
    def _(p):
        gu(1, p)

    x_wait(2)

    @pl.loop(0, 3)
    def _(p):
        gu(2, p)

    w_wait(0, 3, 0)
    to_sib(0, 3)
    w_wait(1, 3, 0)
    to_sib(1, 3)
    d_fwd(0)
    d_start(2)
    w_wait(0, 3, 1)
    w_wait(1, 3, 1)

    @pl.loop(0, 3)
    def _(g):
        gu(g, 3)

    x_wait(3)

    @pl.loop(0, 4)
    def _(p):
        gu(3, p)

    def down(j):
        @pl.loop(0, 4)
        def _(g):
            r = jnp.dot(act[g], wd[j], preferred_element_type=F32).astype(BF16).reshape(4, CAP, CW)
            ob[j, g] = r
            rb[j, 0, g] = r[0]

        for db in (1, 3, 2):
            k, kr = j * 3 + db - 1, j * 3 + (4 - db) % 4 - 1
            go(send(ob.at[j, :, db], rb.at[j, (4 - db) % 4], r1_s.at[k], r1_r.at[kr], ab(0, db)))

    def relay(j):
        for db in (1, 3, 2):
            k = j * 3 + db - 1
            send(ob.at[j, :, db], rb.at[j, db], r1_s.at[k], r1_r.at[k], ab(0, db)).wait_recv()
        for g in (1, 2, 3):
            da = DA[g]
            k, kr = j * 3 + da - 1, j * 3 + (4 - da) % 4 - 1
            go(send(rb.at[j, :, g], ret.at[j, (4 - da) % 4], r2_s.at[k], r2_r.at[kr], ab(da, 0)))
        ret[j, 0] = rb[j, :, 0]

    def combine(j):
        for g in (1, 2, 3):
            da = DA[g]
            k = j * 3 + da - 1
            send(rb.at[j, :, g], ret.at[j, da], r2_s.at[k], r2_r.at[k], ab(da, 0)).wait_recv()
        full = jnp.dot(cm[...], ret[j].reshape(NE * CAP, CW), preferred_element_type=F32)
        total = full[0:TOK] + full[TOK : 2 * TOK] + full[2 * TOK : 3 * TOK]
        comb[:, j * CW : (j + 1) * CW] = total
        return jnp.sum(total * total, axis=-1, keepdims=True)

    d_fwd(1)
    d_start(3)
    d_last(0)
    d_all(0)
    down(0)
    d_last(1)
    d_fwd(2)
    d_all(1)
    down(1)
    d_fwd(3)
    d_last(2)
    d_all(2)
    down(2)
    d_last(3)
    d_all(3)
    down(3)
    sq = jnp.zeros((TOK, 1), F32)
    relay(0)
    relay(1)
    for cp in ogc:
        cp.wait_recv()
    relay(2)
    relay(3)
    for j in range(NCH):
        sq = sq + combine(j)
    scale = lax.rsqrt(sq / D + epsilon)
    for t in range(NT):
        mixed[t] = (comb[:, t * SL : (t + 1) * SL] * scale * og[t]).astype(BF16)
    mine = pl.ds(pl.multiple_of(tp * TOK, TOK), TOK)
    outs = []
    for i in range(1, NT):
        to = (tp + i) % NT
        outs.append(go(send(mixed.at[to], out_ref.at[mine, :], o_s.at[i - 1], o_r.at[i - 1], (ep, to))))
    own = pltpu.make_async_copy(mixed.at[tp], out_ref.at[mine, :], o_l)
    own.start()
    for i in range(1, NT):
        frm = (tp + NT - i) % NT
        theirs = pl.ds(pl.multiple_of(frm * TOK, TOK), TOK)
        send(mixed.at[frm], out_ref.at[theirs, :], o_s.at[i - 1], o_r.at[i - 1], (ep, frm)).wait_recv()
    own.wait()
    for cp in sent:
        cp.wait_send()


def local(tokens, expert_ids, gate_values, norm_gain, gate_weight, up_weight, down_weight, out_gain):
    vm = pl.BlockSpec(memory_space=pltpu.VMEM)
    anym = pl.BlockSpec(memory_space=pltpu.HBM)
    dma = pltpu.SemaphoreType.DMA
    return pl.pallas_call(
        kernel,
        out_shape=jax.ShapeDtypeStruct((NT * TOK, SL), BF16),
        in_specs=[vm, vm, vm, vm, anym, anym, anym, vm],
        out_specs=anym,
        scratch_shapes=[
            pltpu.VMEM((4, D, 512), BF16),
            pltpu.VMEM((NCH, FF, CW), BF16),
            pltpu.VMEM((4, TOK, D), BF16),
            pltpu.VMEM((4, NE, TOK), F32),
            pltpu.VMEM((4, 3, CAP, D), BF16),
            pltpu.VMEM((4, 4, CAP, D), BF16),
            pltpu.VMEM((4, 4 * CAP, FF), BF16),
            pltpu.VMEM((NCH, 4, 4, CAP, CW), BF16),
            pltpu.VMEM((NCH, 4, 4, CAP, CW), BF16),
            pltpu.VMEM((NCH, 4, 4, CAP, CW), BF16),
            pltpu.VMEM((TOK, D), F32),
            pltpu.VMEM((3 * TOK, NE * CAP), BF16),
            pltpu.VMEM((NT, TOK, SL), BF16),
            pltpu.VMEM((NT, 1, SL), F32),
            dma((2 + NCH,)), dma((16,)), dma((16,)), dma((NCH * 9,)), dma((NCH * 9,)),
            dma((8,)), dma((8,)), dma((12,)), dma((12,)),
            dma((NCH * 3,)), dma((NCH * 3,)), dma((NCH * 3,)), dma((NCH * 3,)),
            dma((NT - 1,)), dma((NT - 1,)), dma((NT - 1,)), dma((NT - 1,)), dma(()),
        ],
        compiler_params=pltpu.CompilerParams(
            collective_id=0, has_side_effects=True, vmem_limit_bytes=63000000
        ),
    )(
        tokens, expert_ids.T, gate_values.T, norm_gain.reshape(1, D),
        gate_weight, up_weight, down_weight, out_gain.reshape(1, SL),
    )


def solution(mesh):
    in_specs = (
        P(("ep", "tp"), None), P("ep", None), P("ep", None), P(),
        P("ep", None, "tp"), P("ep", None, "tp"), P("ep", "tp", None), P("tp"),
    )
    return jax.shard_map(
        local, mesh=mesh, in_specs=in_specs, out_specs=P("ep", "tp"), check_vma=False
    )
```
